256 devices in a mesh: ep: 32 (over z, x), tp: 8 (over y, core).
Axes of the slice: x: 4, y: 4, z: 8, core: 2. Of those that a mesh axis runs over, the one named last changes fastest.
Arguments:
- queries: bfloat16 [8192, 2048], P('ep', 'tp'), may hold values from -9 to 9
- keys: bfloat16 [8192, 2048], P('ep', 'tp'), may hold values from -9 to 9
- values: bfloat16 [8192, 2048], P('ep', 'tp'), may hold values from -6 to 6
- lambdas: float32 [16], P('tp'), may hold values from 0.3 to 0.8
- head_gain: float32 [128], replicated, may hold values from 0.1 to 1.9
- moe_input: bfloat16 [32768, 2048], P('ep'), may hold values from -6 to 6
- ffn_gain: float32 [2048], replicated, may hold values from 0.1 to 1.9
- group_router: bfloat16 [2048, 4], replicated, may hold values from -0.125 to 0.125
- expert_router: bfloat16 [2048, 32], replicated, may hold values from -0.125 to 0.125
- routes: int32 [32768, 2], P('ep'), may hold values from 0 to 31, as said below
- w_gate: bfloat16 [32, 2048, 1024], P('ep', None, 'tp'), may hold values from -0.125 to 0.125
- w_up: bfloat16 [32, 2048, 1024], P('ep', None, 'tp'), may hold values from -0.125 to 0.125
- w_down: bfloat16 [32, 1024, 2048], P('ep', 'tp'), may hold values from -0.1875 to 0.1875
Outputs:
- attn_out: bfloat16 [8192, 2048], P('ep', 'tp')
- moe_out: bfloat16 [32768, 2048], P(('ep', 'tp'))
The draws below stay inside these ranges and needn't reach their ends.
Inputs may be any that keep to these rules, and one draw needn't show every extreme that they name: `routes`: in each aligned block of 128 rows (the rows of one device) every expert is named by exactly 8 rows and every group by the same number of rows; a row's two experts differ and lie in one group of 8 consecutive expert numbers.
All inputs are finite; a program needn't handle non-finite values.
Results may differ from the reference program's by a relative error of at most 0.015.
Values may be sent and summed in bfloat16 or wider, within the bound.
No kernel may reach another device: no remote copies, remote signals or barrier semaphores. Data moves between devices by JAX's collectives and lax.ppermute only.
A program may use at most 128 MiB of HBM per device.

```python
import jax
import jax.numpy as jnp
from jax import lax

D = 2048
HEADS = 16
QK_DIM = 64
V_DIM = 128
FF = 1024
GROUPS = 4
TOPK = 2
ROWS = 128
EXPERTS = 32
GROUP_SIZE = 8
FF_PART = 128
TOK_A = 8192
TOK_B = 32768
N_TP = 8


def draw_queries(key, part):
    shape = (TOK_A, HEADS * 2 * QK_DIM)
    drawn = jnp.clip(1.3 * jax.random.normal(jax.random.fold_in(key, 1), shape, jnp.float32), -6.0, 6.0)
    return drawn.astype(jnp.bfloat16)


def draw_keys(key, part):
    shape = (TOK_A, HEADS * 2 * QK_DIM)
    drawn = jnp.clip(1.3 * jax.random.normal(jax.random.fold_in(key, 2), shape, jnp.float32), -6.0, 6.0)
    return drawn.astype(jnp.bfloat16)


def draw_routes(key, part):
    block_count = TOK_B // ROWS
    per_group = ROWS // GROUPS
    block_keys = jax.random.split(jax.random.fold_in(key, 11), block_count)

    def one_block(block_key):
        place_key, group_key, expert_key, order_key = jax.random.split(block_key, 4)
        places = jax.random.permutation(place_key, ROWS)
        group_index = places // per_group
        inner_index = places % per_group
        first_pick = inner_index % GROUP_SIZE
        shift_amount = 1 + inner_index // GROUP_SIZE % (GROUP_SIZE - 1)
        second_pick = (first_pick + shift_amount) % GROUP_SIZE
        group_labels = jax.random.permutation(group_key, GROUPS)[group_index]
        expert_orders = jax.vmap(lambda inner_key: jax.random.permutation(inner_key, GROUP_SIZE))(jax.random.split(expert_key, GROUPS))
        first_expert = expert_orders[group_index, first_pick]
        second_expert = expert_orders[group_index, second_pick]
        flips = jax.random.randint(order_key, (ROWS,), 0, 2)
        lead_expert = jnp.where(flips == 1, second_expert, first_expert)
        tail_expert = jnp.where(flips == 1, first_expert, second_expert)
        base_number = group_labels * GROUP_SIZE
        return jnp.stack([base_number + lead_expert, base_number + tail_expert], axis=1)
    return jax.vmap(one_block)(block_keys).reshape(TOK_B, TOPK).astype(jnp.int32)


def shard_levels(key, extent, cuts, low, largest):
    level = 1.0
    for position, parts in cuts:
        draws = jax.random.uniform(jax.random.fold_in(jax.random.fold_in(key, 6), position), (parts,), jnp.float32, low / len(cuts), largest / len(cuts))
        level = level * jnp.repeat(jnp.exp(draws), extent[position] // parts).reshape((-1,) + (1,) * (len(extent) - 1 - position))
    return level


def centred(key, dims, spread, limit, shards=(), kind=jnp.bfloat16):
    entries = spread * jax.random.normal(key, dims, jnp.float32)
    if shards:
        entries = entries * shard_levels(key, dims, shards, -0.22, 0.18)
    return jnp.clip(entries, -limit, limit).astype(kind)


def setup_inputs(seed: int = 0) -> dict:
    key_list = jax.random.split(jax.random.key(seed), 14)
    queries = draw_queries(jax.random.fold_in(key_list[13], 71), 0)
    keys = draw_keys(jax.random.fold_in(key_list[13], 71), 0)
    values = centred(key_list[2], (TOK_A, HEADS * V_DIM), 1.0, 6.0, ((0, 32), (1, 8)))
    lambdas = jnp.clip(0.3 + 0.5 * jax.random.uniform(key_list[3], (HEADS,), jnp.float32) ** shard_levels(key_list[3], (HEADS,), ((0, 8),), -0.2, 0.2), 0.3, 0.8)
    head_gain = jnp.clip(1.0 + 0.18 * jax.random.normal(key_list[4], (V_DIM,), jnp.float32), 0.1, 1.9)
    moe_input = centred(key_list[5], (TOK_B, D), 1.0, 6.0, ((0, 32),))
    ffn_gain = jnp.clip(1.0 + 0.18 * jax.random.normal(key_list[6], (D,), jnp.float32), 0.1, 1.9)
    group_router = centred(key_list[7], (D, GROUPS), D ** -0.5, 0.125)
    expert_router = centred(key_list[8], (D, EXPERTS), D ** -0.5, 0.125)
    routes = draw_routes(jax.random.fold_in(key_list[13], 71), 0)
    w_gate = centred(key_list[10], (EXPERTS, D, FF), D ** -0.5, 0.125, ((0, 32), (2, 8)))
    w_up = centred(key_list[11], (EXPERTS, D, FF), D ** -0.5, 0.125, ((0, 32), (2, 8)))
    w_down = centred(key_list[12], (EXPERTS, FF, D), FF ** -0.5, 0.1875, ((0, 32), (1, 8)))
    return {"queries": queries, "keys": keys, "values": values, "lambdas": lambdas, "head_gain": head_gain, "moe_input": moe_input, "ffn_gain": ffn_gain, "group_router": group_router, "expert_router": expert_router, "routes": routes, "w_gate": w_gate, "w_up": w_up, "w_down": w_down}


norm_eps = 1e-06

def rms_scaled(rows, gain):
    widened = rows.astype(jnp.float32)
    return widened * lax.rsqrt(lax.optimization_barrier(jnp.mean(widened * widened, axis=-1, keepdims=True)) + norm_eps) * gain

def route_gates(normed, own_routes, group_router, expert_router):
    group_count = group_router.shape[1]
    expert_count = expert_router.shape[1]
    group_logits = jnp.dot(normed, group_router, preferred_element_type=jnp.float32)
    expert_logits = jnp.dot(normed, expert_router, preferred_element_type=jnp.float32)
    chosen = own_routes[:, 0] // (expert_count // group_count)
    group_mask = jnp.arange(group_count, dtype=jnp.int32)[None, :] == chosen[:, None]
    own_logit = lax.optimization_barrier(jnp.sum(jnp.where(group_mask, group_logits, 0.0), axis=-1, keepdims=True))
    group_share = 1.0 / lax.optimization_barrier(jnp.sum(jnp.exp(group_logits - own_logit), axis=-1))
    expert_mask = jnp.arange(expert_count, dtype=jnp.int32)[None, None, :] == own_routes[:, :, None]
    picked = lax.optimization_barrier(jnp.sum(jnp.where(expert_mask, expert_logits[:, None, :], 0.0), axis=-1))
    return group_share[:, None] * jax.nn.sigmoid(picked - picked[:, ::-1])

def attention_part(queries, keys, values, lambdas, head_gain):
    row_count = queries.shape[0]
    query_heads = queries.reshape(row_count, HEADS, 2, QK_DIM).astype(jnp.float32).transpose(1, 0, 2, 3)
    key_heads = keys.reshape(row_count, HEADS, 2, QK_DIM).astype(jnp.float32).transpose(1, 0, 2, 3)
    value_heads = values.reshape(row_count, HEADS, V_DIM).transpose(1, 0, 2)
    positions = jnp.arange(row_count, dtype=jnp.int32)
    allowed = positions[None, :] <= positions[:, None]

    def one_head(pack):
        query_one, key_one, value_one, weight_one = pack
        scores = jnp.einsum('qmd,kmd->mqk', query_one, key_one) * QK_DIM ** (-0.5)
        scores = jnp.where(allowed, scores, -jnp.inf)
        maxima = lax.optimization_barrier(jnp.max(scores, axis=-1, keepdims=True))
        exp_terms = jnp.where(allowed, jnp.exp(scores - maxima), 0.0)
        shares = exp_terms / lax.optimization_barrier(jnp.sum(exp_terms, axis=-1, keepdims=True))
        mixed = (shares[0] - weight_one * shares[1]).astype(jnp.bfloat16)
        return jnp.dot(mixed, value_one, preferred_element_type=jnp.float32)
    heads_out = lax.map(one_head, (query_heads, key_heads, value_heads, lambdas))
    normed = rms_scaled(heads_out, head_gain).astype(jnp.bfloat16)
    return normed.transpose(1, 0, 2).reshape(row_count, HEADS * V_DIM)

def expert_part(moe_input, ffn_gain, group_router, expert_router, routes, w_gate, w_up, w_down):
    normed = rms_scaled(moe_input, ffn_gain).astype(jnp.bfloat16)
    gates = route_gates(normed, routes, group_router, expert_router)
    flat_routes = routes.reshape(-1)
    sorted_order = jnp.argsort(flat_routes, stable=True).astype(jnp.int32)
    per_expert = flat_routes.shape[0] // EXPERTS
    sorted_rows = normed[sorted_order // 2].reshape(EXPERTS, per_expert, D)

    def one_expert(pack):
        expert_rows, gate_weight, up_weight, down_weight = pack
        gate_part = jnp.dot(expert_rows, gate_weight, preferred_element_type=jnp.float32)
        up_part = jnp.dot(expert_rows, up_weight, preferred_element_type=jnp.float32)
        hidden = (jax.nn.silu(gate_part) * up_part).astype(jnp.bfloat16)
        pieces = hidden.reshape(per_expert, N_TP, FF_PART).astype(jnp.float32)
        down_parts = down_weight.reshape(N_TP, FF_PART, D).astype(jnp.float32)
        partial_value = jnp.einsum('nsf,sfd->snd', pieces, down_parts).astype(jnp.bfloat16)
        partial_value = lax.optimization_barrier(partial_value)
        return lax.optimization_barrier(jnp.sum(partial_value.astype(jnp.float32), axis=0)).astype(jnp.bfloat16)
    outputs = lax.map(one_expert, (sorted_rows, w_gate, w_up, w_down)).reshape(-1, D)
    placed = jnp.zeros_like(outputs).at[sorted_order].set(outputs)
    per_token = placed.reshape(-1, 2, D).astype(jnp.float32)
    return lax.optimization_barrier(jnp.sum(per_token * gates[..., None], axis=1)).astype(jnp.bfloat16)

def reference(queries, keys, values, lambdas, head_gain, moe_input, ffn_gain, group_router, expert_router, routes, w_gate, w_up, w_down):
    attn_out = attention_part(queries, keys, values, lambdas, head_gain)
    moe_out = expert_part(moe_input, ffn_gain, group_router, expert_router, routes, w_gate, w_up, w_down)
    return (attn_out, moe_out)
```

```python
import functools
import math

import jax
import jax.numpy as jnp
from jax import lax
from jax.experimental import pallas as pl
from jax.experimental.pallas import tpu as pltpu
from jax.sharding import Mesh
from jax.sharding import PartitionSpec as P


EP = ("z", "x")
EP_TP = ("z", "x", "y", "c")
TP = ("y", "c")

norm_eps = 1e-06
masked_score = -1e30
VMEM_LIMIT = 56 * 1024 * 1024
F32 = jnp.float32
BF16 = jnp.bfloat16


def shifted(array, axis, by):
    n = lax.axis_size(axis)
    return lax.ppermute(array, axis, [(i, (i + by) % n) for i in range(n)])


def whole(shape):
    return pl.BlockSpec(shape, lambda *_: (0,) * len(shape))


def slot_masks(routes_t, expert_count, capacity):
    tokens = routes_t.shape[1]
    experts = lax.broadcasted_iota(jnp.int32, (expert_count, tokens), 0)
    named = [routes_t[k : k + 1, :] == experts for k in range(2)]
    both = jnp.where(named[0] | named[1], 1.0, 0.0).astype(BF16)
    earlier = jnp.where(
        lax.broadcasted_iota(jnp.int32, (tokens, tokens), 0)
        < lax.broadcasted_iota(jnp.int32, (tokens, tokens), 1),
        1.0,
        0.0,
    ).astype(BF16)
    rank = jnp.dot(both, earlier, preferred_element_type=F32).astype(jnp.int32)
    place = lax.broadcasted_iota(jnp.int32, (expert_count, capacity, tokens), 1)
    rank = jnp.broadcast_to(rank[:, None, :], place.shape)
    masks = []
    for k in range(2):
        hit = jnp.broadcast_to(jnp.where(named[k], 1, 0)[:, None, :], place.shape)
        masks.append(((hit == 1) & (rank == place)).reshape(expert_count * capacity, tokens))
    return masks


def dispatch_kernel(which, rows_ref, gain_ref, routes_ref, normed_ref, packed_ref, *, experts, capacity):
    rows = rows_ref[...].astype(F32)
    inv = lax.rsqrt(jnp.mean(rows * rows, axis=-1, keepdims=True) + norm_eps)
    normed = (rows * inv * gain_ref[...]).astype(BF16)
    normed_ref[...] = normed
    first, second = slot_masks(routes_ref[...], experts, capacity)
    pick = jnp.where(first | second, 1.0, 0.0).astype(BF16)
    packed_ref[...] = jnp.dot(pick, normed, preferred_element_type=F32).astype(BF16)


def dispatch(tp_index, moe_input, ffn_gain, routes_t, own_count, experts, capacity):
    width = moe_input.shape[1]
    return pl.pallas_call(
        functools.partial(dispatch_kernel, experts=experts, capacity=capacity),
        grid_spec=pltpu.PrefetchScalarGridSpec(
            num_scalar_prefetch=1,
            grid=(1,),
            in_specs=[
                pl.BlockSpec((own_count, width), lambda i, w: (w[0], 0)),
                pl.BlockSpec((1, width), lambda i, w: (0, 0)),
                pl.BlockSpec((2, own_count), lambda i, w: (0, w[0])),
            ],
            out_specs=[
                pl.BlockSpec((own_count, width), lambda i, w: (0, 0)),
                pl.BlockSpec((experts * capacity, width), lambda i, w: (0, 0)),
            ],
        ),
        out_shape=[
            jax.ShapeDtypeStruct((own_count, width), BF16),
            jax.ShapeDtypeStruct((experts * capacity, width), BF16),
        ],
        compiler_params=pltpu.CompilerParams(vmem_limit_bytes=VMEM_LIMIT),
        name="dispatch",
    )(tp_index.reshape(1), moe_input, ffn_gain.reshape(1, -1), routes_t)


def combine_kernel(which, homed_ref, gates_ref, routes_ref, out_ref, *, experts, capacity):
    first, second = slot_masks(routes_ref[...], experts, capacity)
    gates = gates_ref[...]
    weights = jnp.where(first, gates[0:1, :], 0.0) + jnp.where(second, gates[1:2, :], 0.0)
    weights = weights.T
    high = weights.astype(BF16)
    low = (weights - high.astype(F32)).astype(BF16)
    homed = homed_ref[...]
    out = jnp.dot(high, homed, preferred_element_type=F32)
    out += jnp.dot(low, homed, preferred_element_type=F32)
    out_ref[...] = out.astype(BF16)


def combine(tp_index, homed, gates_t, routes_t, own_count, experts, capacity):
    width = homed.shape[1]
    return pl.pallas_call(
        functools.partial(combine_kernel, experts=experts, capacity=capacity),
        grid_spec=pltpu.PrefetchScalarGridSpec(
            num_scalar_prefetch=1,
            grid=(1,),
            in_specs=[
                pl.BlockSpec((experts * capacity, width), lambda i, w: (0, 0)),
                pl.BlockSpec((2, own_count), lambda i, w: (0, 0)),
                pl.BlockSpec((2, own_count), lambda i, w: (0, w[0])),
            ],
            out_specs=pl.BlockSpec((own_count, width), lambda i, w: (0, 0)),
        ),
        out_shape=jax.ShapeDtypeStruct((own_count, width), BF16),
        compiler_params=pltpu.CompilerParams(vmem_limit_bytes=VMEM_LIMIT),
        name="combine",
    )(tp_index.reshape(1), homed, gates_t, routes_t)


def route_gates(normed, own_routes, group_router, expert_router):
    group_count = group_router.shape[1]
    expert_count = expert_router.shape[1]
    group_logits = jnp.dot(normed, group_router, preferred_element_type=F32)
    expert_logits = jnp.dot(normed, expert_router, preferred_element_type=F32)
    chosen = own_routes[:, 0] // (expert_count // group_count)
    group_mask = jnp.arange(group_count, dtype=jnp.int32)[None, :] == chosen[:, None]
    own_logit = jnp.sum(jnp.where(group_mask, group_logits, 0.0), axis=-1, keepdims=True)
    group_share = 1.0 / jnp.sum(jnp.exp(group_logits - own_logit), axis=-1)
    expert_mask = jnp.arange(expert_count, dtype=jnp.int32)[None, None, :] == own_routes[:, :, None]
    picked = jnp.sum(jnp.where(expert_mask, expert_logits[:, None, :], 0.0), axis=-1)
    return group_share[:, None] * jax.nn.sigmoid(picked - picked[:, ::-1])


def call(body, args, outs, specs=None, prefetch=None):
    in_specs = [whole(a.shape) for a in args] if specs is None else specs
    out_specs = [whole(o.shape) for o in outs]
    grid_spec = pltpu.PrefetchScalarGridSpec(
        num_scalar_prefetch=0 if prefetch is None else 1,
        grid=(1,),
        in_specs=in_specs,
        out_specs=out_specs,
    )
    operands = args if prefetch is None else (prefetch, *args)
    return pl.pallas_call(
        body,
        grid_spec=grid_spec,
        out_shape=list(outs),
        compiler_params=pltpu.CompilerParams(vmem_limit_bytes=VMEM_LIMIT),
    )(*operands)


def pack_weights_kernel(gate_ref, up_ref, down_ref, top_ref, bottom_ref):
    rows, lanes = gate_ref.shape
    extra = top_ref.shape[0] - rows
    top_ref[:rows, :] = gate_ref[...]
    top_ref[rows:, :] = up_ref[:extra, :]
    bottom_ref[: rows - extra, :] = up_ref[extra:, :]
    at = rows - extra
    for n in range(down_ref.shape[1] // lanes):
        bottom_ref[at : at + lanes, :] = down_ref[:, n * lanes : (n + 1) * lanes]
        at += lanes


def pack_weights(gate, up, down):
    rows, lanes = gate.shape
    shape = jax.ShapeDtypeStruct((3 * rows // 2, lanes), BF16)
    return call(pack_weights_kernel, (gate, up, down), (shape, shape))


def ffn_kernel(*refs, parts):
    mine_ref, other_ref = refs[:2]
    tops, bottoms = refs[2 : 2 + parts], refs[2 + parts : 2 + 2 * parts]
    own_out, other_out = refs[2 + 2 * parts :]
    model = mine_ref.shape[1]
    lanes = tops[0].shape[1]
    extra = tops[0].shape[0] - model
    for rows_ref, out_ref in ((mine_ref, own_out), (other_ref, other_out)):
        rows = rows_ref[...]
        hidden = []
        for top, bottom in zip(tops, bottoms):
            gate = top[:model, :]
            up = jnp.concatenate([top[model:, :], bottom[: model - extra, :]], axis=0)
            gate_up = jnp.dot(
                rows, jnp.concatenate([gate, up], axis=1), preferred_element_type=F32
            )
            g, u = gate_up[:, :lanes], gate_up[:, lanes:]
            hidden.append((g / (1.0 + jnp.exp(-g)) * u).astype(BF16))
        hidden = jnp.concatenate(hidden, axis=1)
        for n in range(model // (2 * lanes)):
            at = model - extra + 2 * n * lanes
            block = jnp.concatenate(
                [
                    jnp.concatenate([b[at : at + lanes, :], b[at + lanes : at + 2 * lanes, :]], axis=1)
                    for b in bottoms
                ],
                axis=0,
            )
            out_ref[:, 2 * n * lanes : 2 * (n + 1) * lanes] = jnp.dot(
                hidden, block, preferred_element_type=F32
            ).astype(out_ref.dtype)


def ffn(mine, other, tops, bottoms):
    return call(
        functools.partial(ffn_kernel, parts=len(tops)),
        (mine, other, *tops, *bottoms),
        (jax.ShapeDtypeStruct(mine.shape, BF16), jax.ShapeDtypeStruct(mine.shape, BF16)),
    )


Q_CHUNK = 256
OFFSETS = (0, -1, 1, -2, 2, -3, 3, 4)


def pack_heads_kernel(where_ref, q_ref, k_ref, v_ref, *outs, half, depth):
    for n, out in enumerate(outs):
        pick = lax.rem(where_ref[1] - n + 4, 4)
        at = pl.ds(pl.multiple_of((pick // 2) * depth, depth), depth)
        rows = pl.ds(pl.multiple_of(lax.rem(pick, 2) * half, half), half)
        out[:, :depth] = k_ref[rows, at]
        out[:, depth : 2 * depth] = v_ref[rows, at]
        out[:, 2 * depth : 3 * depth] = q_ref[:half, at]
        out[:, 3 * depth :] = q_ref[half:, at]


def sort_heads_kernel(where_ref, *refs, half, depth):
    messages, (q_out, kv_out) = refs[:4], refs[4:]
    first = 2 * lax.rem(where_ref[1], 2) + where_ref[2]
    for n, message in enumerate(messages):
        at = pl.ds(pl.multiple_of(lax.rem(first + n, 4) * half, half), half)
        kv_out[at, :] = message[:, : 2 * depth]
        q_out[0, at, :] = message[:, 2 * depth : 3 * depth]
        q_out[1, at, :] = message[:, 3 * depth :]


def attend_kernel(where_ref, q_ref, *refs, slices, half, scale):
    blocks = refs[:slices]
    far_low = refs[slices]
    own_ref, other_ref, kv, acc, top_ref, sems = refs[slices + 1 :]
    z, core = where_ref[0], where_ref[2]
    keys, two_depth = blocks[0].shape
    depth = two_depth // 2
    width = depth // 2
    rows = q_ref.shape[1]
    copies = []
    for n, (offset, block) in enumerate(zip(OFFSETS, blocks)):
        source = lax.rem(z + offset + slices, slices) * keys
        copies.append(
            pltpu.make_async_copy(
                block, kv.at[pl.ds(pl.multiple_of(source, keys), block.shape[0]), :], sems.at[n]
            )
        )
        if n == slices - 1:
            copies.append(
                pltpu.make_async_copy(
                    far_low,
                    kv.at[
                        pl.ds(
                            pl.multiple_of(source + block.shape[0], block.shape[0]),
                            block.shape[0],
                        ),
                        :,
                    ],
                    sems.at[n + 1],
                )
            )
    for copy in copies:
        copy.start()
    for copy in copies:
        copy.wait()

    per_side = rows // Q_CHUNK

    def fold(q, first_key, count, q_first, q_half, diagonal):
        at = pl.ds(pl.multiple_of(first_key, keys), count)
        v = jnp.concatenate([kv[at, depth:], jnp.ones((count, depth), BF16)], axis=1)
        if diagonal:
            qi = lax.broadcasted_iota(jnp.int32, (Q_CHUNK, count), 0) + q_first
            ki = lax.broadcasted_iota(jnp.int32, (Q_CHUNK, count), 1)
            k_pos = (ki // half) * (2 * half) + core * half + ki % half
            q_pos = (qi // half) * (2 * half) + q_half * half + qi % half
            allowed = k_pos <= q_pos
        for m in range(2):
            s = lax.dot_general(
                q[:, m * width : (m + 1) * width],
                kv[at, m * width : (m + 1) * width],
                (((1,), (1,)), ((), ())),
                preferred_element_type=F32,
            )
            if diagonal:
                s = jnp.where(allowed, s, masked_score)
            top = jnp.max(s, axis=1, keepdims=True)
            if not diagonal:
                old = top_ref[m, :, :1]
                top = jnp.maximum(top, old)
                keep = jnp.exp2((old - top) * scale)
            e = jnp.exp2((s - top) * scale)
            if diagonal:
                e = jnp.where(allowed, e, 0.0)
            mixed = jnp.dot(e.astype(BF16), v, preferred_element_type=F32)
            if not diagonal:
                mixed = mixed + acc[m] * keep
            acc[m] = mixed
            top_ref[m] = jnp.broadcast_to(top, top_ref.shape[1:])

    def chunk(n, carry):
        side = n // per_side
        q_first = pl.multiple_of(lax.rem(n, per_side) * Q_CHUNK, Q_CHUNK)
        q_half = jnp.where(side == 0, core, 1 - core)
        q = q_ref[q_half, pl.ds(q_first, Q_CHUNK), :]
        fold(q, z * keys, keys, q_first, q_half, True)

        def pair(p, c):
            fold(q, p * 2 * keys, 2 * keys, q_first, q_half, False)
            return c

        lax.fori_loop(0, z // 2, pair, 0)

        @pl.when(lax.rem(z, 2) == 1)
        def _():
            fold(q, (z - 1) * keys, keys, q_first, q_half, False)

        at = pl.ds(q_first, Q_CHUNK)
        for chosen, ref in ((0, own_ref), (1, other_ref)):

            @pl.when(side == chosen)
            def _(ref=ref):
                for m in range(2):
                    ref[m, at, :depth] = acc[m, :, :depth]
                    ref[m, at, depth:] = jnp.concatenate(
                        [top_ref[m, :, : depth // 2], acc[m, :, depth : depth + depth // 2]], axis=1
                    )

        return carry

    lax.fori_loop(0, 2 * per_side, chunk, 0)


def attend(where, q, blocks, far_low, half, scale):
    rows, depth = q.shape[1:]
    slices = len(blocks)
    keys = blocks[0].shape[0]
    part = jax.ShapeDtypeStruct((2, rows, 2 * depth), F32)
    return pl.pallas_call(
        functools.partial(attend_kernel, slices=slices, half=half, scale=scale),
        grid_spec=pltpu.PrefetchScalarGridSpec(
            num_scalar_prefetch=1,
            grid=(1,),
            in_specs=[whole(q.shape)]
            + [pl.BlockSpec(memory_space=pl.ANY)] * (slices + 1),
            out_specs=[whole(part.shape)] * 2,
            scratch_shapes=[
                pltpu.VMEM((slices * keys, 2 * depth), BF16),
                pltpu.VMEM((2, Q_CHUNK, 2 * depth), F32),
                pltpu.VMEM((2, Q_CHUNK, depth), F32),
                pltpu.SemaphoreType.DMA((slices + 1,)),
            ],
        ),
        out_shape=[part, part],
        compiler_params=pltpu.CompilerParams(vmem_limit_bytes=VMEM_LIMIT),
        name="attend",
    )(where, q, *blocks, far_low)


def merge_kernel(where_ref, mine_ref, theirs_ref, weight_ref, gain_ref, *outs, scale):
    depth = gain_ref.shape[1]
    half = outs[0].shape[0]
    first = 2 * lax.rem(where_ref[1], 2) + where_ref[2]
    head = lax.rem(where_ref[1], 2)
    weight = jnp.where(where_ref[1] // 2 == where_ref[2], weight_ref[head], weight_ref[2 + head])
    for n, out_ref in enumerate(outs):
        at = pl.ds(pl.multiple_of(lax.rem(first + n, 4) * half, half), half)
        heads = []
        for m in range(2):
            mine, theirs = mine_ref[m, at, :], theirs_ref[m, at, :]
            top_a, top_b = mine[:, depth : depth + 1], theirs[:, depth : depth + 1]
            total_a = mine[:, depth + depth // 2 : depth + depth // 2 + 1]
            total_b = theirs[:, depth + depth // 2 : depth + depth // 2 + 1]
            top = jnp.maximum(top_a, top_b)
            keep_a = jnp.exp2((top_a - top) * scale)
            keep_b = jnp.exp2((top_b - top) * scale)
            total = total_a * keep_a + total_b * keep_b
            heads.append(mine[:, :depth] * (keep_a / total) + theirs[:, :depth] * (keep_b / total))
        out = heads[0] - weight * heads[1]
        out = out * lax.rsqrt(jnp.mean(out * out, axis=1, keepdims=True) + norm_eps)
        out_ref[...] = (out * gain_ref[...]).astype(BF16)


def merge(where, mine, theirs, weights, head_gain, half, scale):
    depth = head_gain.shape[0]
    args = (mine, theirs, weights, head_gain.reshape(1, depth))
    specs = [whole(a.shape) for a in args]
    specs[2] = pl.BlockSpec(memory_space=pltpu.SMEM)
    return call(
        functools.partial(merge_kernel, scale=scale),
        args,
        [jax.ShapeDtypeStruct((half, depth), BF16)] * 4,
        specs=specs,
        prefetch=where,
    )


def lay_out_kernel(where_ref, *refs):
    out = refs[4]
    half, depth = refs[0].shape
    for n, message in enumerate(refs[:4]):
        pick = lax.rem(where_ref[1] - n + 4, 4)
        rows = pl.ds(pl.multiple_of(lax.rem(pick, 2) * half, half), half)
        out[rows, pl.ds(pl.multiple_of((pick // 2) * depth, depth), depth)] = message[...]


def ring_pairs(step, size):
    pairs = []
    for target in range(size):
        source = (target - (1 if step > 0 else -1)) % size
        moved = (target - step) % size
        for hop in range(size):
            reader = (target + (hop if step > 0 else -hop)) % size
            distance = abs(step) + hop
            limit = 4
            if distance <= limit and moved < reader:
                pairs.append((source, target))
                break
    return pairs


def local(
    queries,
    keys,
    values,
    lambdas,
    head_gain,
    moe_input,
    ffn_gain,
    group_router,
    expert_router,
    routes,
    w_gate,
    w_up,
    w_down,
):
    z, x, _, core = (lax.axis_index(a) for a in EP_TP)
    tp_index = lax.axis_index(TP)
    where = jnp.stack([z, x, core])

    top, bottom = pack_weights(w_gate[0], w_up[0], w_down[0])
    top_f = shifted(top, "y", 1)
    bottom_b = shifted(bottom, "y", -1)
    bottom_f = shifted(bottom, "y", 1)
    top_b = shifted(top, "y", -1)
    top_o = shifted(top_f, "y", 1)
    bottom_o = shifted(bottom_b, "y", -1)

    rows = queries.shape[0]
    half = rows // 2
    depth = head_gain.shape[0]
    scale = math.log2(math.e) * (depth // 2) ** (-0.5)
    message = jax.ShapeDtypeStruct((half, 4 * depth), BF16)
    messages = call(
        functools.partial(pack_heads_kernel, half=half, depth=depth),
        (queries, keys, values),
        [message] * 4,
        prefetch=where,
    )

    def head_pairs(n, back=False):
        pairs = []
        for sx in range(4):
            for sc in range(2):
                pick = (sx - n) % 4
                here, there = sx * 2 + sc, (2 * sc + pick // 2) * 2 + pick % 2
                pairs.append((there, here) if back else (here, there))
        return pairs

    received = []
    for n, m in enumerate(messages):
        received.append(lax.ppermute(m, ("x", "c"), head_pairs(n)))
    q, kv = call(
        functools.partial(sort_heads_kernel, half=half, depth=depth),
        tuple(received),
        (
            jax.ShapeDtypeStruct((2, 4 * half, depth), BF16),
            jax.ShapeDtypeStruct((4 * half, 2 * depth), BF16),
        ),
        prefetch=where,
    )

    def ring(array, step):
        return lax.ppermute(array, "z", ring_pairs(step, lax.axis_size("z")))

    f1, b1 = ring(kv, 1), ring(kv, -1)
    f2, b2 = ring(f1, 2), ring(b1, -2)
    f3, b3 = ring(f2, 3), ring(b2, -3)
    mid = kv.shape[0] // 2
    far_high, far_low = ring(f3[:mid], 4), ring(b3[mid:], -4)
    all_lambdas = jnp.concatenate([lambdas, shifted(lambdas, "c", 1)])

    own_count = routes.shape[0] // lax.axis_size(TP)
    experts = expert_router.shape[1]
    capacity = 2 * own_count // experts
    model_width = moe_input.shape[1]
    routes_t = routes.T
    normed, packed = dispatch(tp_index, moe_input, ffn_gain, routes_t, own_count, experts, capacity)
    arrived = lax.all_to_all(
        packed.reshape(experts, capacity, model_width), EP, split_axis=0, concat_axis=0, tiled=True
    ).reshape(experts * capacity, model_width)
    other_rows = shifted(arrived, "c", 1)
    mine, theirs = ffn(
        arrived,
        other_rows,
        (top, top_f, top_b, top_o),
        (bottom, bottom_f, bottom_b, bottom_o),
    )
    results = mine + shifted(theirs, "c", 1)
    homed = lax.all_to_all(
        results.reshape(experts, capacity, model_width), EP, split_axis=0, concat_axis=0, tiled=True
    ).reshape(experts * capacity, model_width)

    part_own, part_other = attend(
        where, q, (kv, f1, b1, f2, b2, f3, b3, far_high), far_low, half, scale
    )
    part_got = shifted(part_other, "c", 1)
    outgoing = merge(where, part_own, part_got, all_lambdas, head_gain, half, scale)
    incoming = []
    for n, m in enumerate(outgoing):
        incoming.append(lax.ppermute(m, ("x", "c"), head_pairs(n, back=True)))
    (attn_out,) = call(
        lay_out_kernel,
        tuple(incoming),
        [jax.ShapeDtypeStruct((rows, queries.shape[1]), BF16)],
        prefetch=where,
    )

    own_routes = lax.dynamic_slice_in_dim(routes, tp_index * own_count, own_count, 0)
    gates = route_gates(normed, own_routes, group_router, expert_router)
    moe_out = combine(tp_index, homed, gates.T, routes_t, own_count, experts, capacity)
    return (attn_out, moe_out)


def solution(mesh):
    split = Mesh(mesh.devices.reshape(8, 4, 4, 2), EP_TP)
    placed = (
        P(EP, TP),
        P(EP, TP),
        P(EP, TP),
        P(TP),
        P(),
        P(EP, None),
        P(),
        P(),
        P(),
        P(EP, None),
        P(EP, None, TP),
        P(EP, None, TP),
        P(EP, TP, None),
    )

    return jax.shard_map(
        local, mesh=split, in_specs=placed, out_specs=(P(EP, TP), P(EP_TP, None)), check_vma=False
    )
```

```python
import functools
import math

import jax
import jax.numpy as jnp
from jax import lax
from jax.experimental import pallas as pl
from jax.experimental.pallas import tpu as pltpu
from jax.sharding import Mesh
from jax.sharding import PartitionSpec as P


EP = ("z", "x")
EP_TP = ("z", "x", "y", "c")
TP = ("y", "c")

norm_eps = 1e-06
masked_score = -1e30
F32 = jnp.float32
BF16 = jnp.bfloat16
WIDE = 56 * 1024 * 1024


def shifted(array, axis, by):
    n = lax.axis_size(axis)
    return lax.ppermute(array, axis, [(i, (i + by) % n) for i in range(n)])


def windowed(body, args, outs, scalars, specs=None):
    def whole(shape):
        return pl.BlockSpec(shape, lambda *_: (0,) * len(shape))

    return pl.pallas_call(
        body,
        grid_spec=pltpu.PrefetchScalarGridSpec(
            num_scalar_prefetch=len(scalars),
            grid=(1,),
            in_specs=[whole(a.shape) for a in args] if specs is None else specs,
            out_specs=[whole(o.shape) for o in outs],
        ),
        out_shape=list(outs),
        compiler_params=pltpu.CompilerParams(vmem_limit_bytes=WIDE),
    )(*scalars, *args)


def call(body, args, outs, scalars=(), streamed=(), scratch=(), vmem=8 * 1024 * 1024):
    return pl.pallas_call(
        body,
        in_specs=[pl.BlockSpec(memory_space=pltpu.SMEM)] * len(scalars)
        + [pl.BlockSpec(memory_space=pltpu.HBM)] * len(streamed)
        + [pl.BlockSpec(memory_space=pltpu.VMEM)] * len(args),
        out_specs=[pl.BlockSpec(memory_space=pltpu.VMEM)] * len(outs),
        out_shape=list(outs),
        scratch_shapes=list(scratch),
        compiler_params=pltpu.CompilerParams(vmem_limit_bytes=vmem),
    )(*scalars, *streamed, *args)


def slot_masks(routes_t, expert_count, capacity):
    tokens = routes_t.shape[1]
    experts = lax.broadcasted_iota(jnp.int32, (expert_count, tokens), 0)
    named = [routes_t[k : k + 1, :] == experts for k in range(2)]
    both = jnp.where(named[0] | named[1], 1.0, 0.0).astype(BF16)
    earlier = jnp.where(
        lax.broadcasted_iota(jnp.int32, (tokens, tokens), 0)
        < lax.broadcasted_iota(jnp.int32, (tokens, tokens), 1),
        1.0,
        0.0,
    ).astype(BF16)
    rank = jnp.dot(both, earlier, preferred_element_type=F32).astype(jnp.int32)
    place = lax.broadcasted_iota(jnp.int32, (expert_count, capacity, tokens), 1)
    rank = jnp.broadcast_to(rank[:, None, :], place.shape)
    masks = []
    for k in range(2):
        hit = jnp.broadcast_to(jnp.where(named[k], 1, 0)[:, None, :], place.shape)
        masks.append(((hit == 1) & (rank == place)).reshape(expert_count * capacity, tokens))
    return masks


def own_routes(tp_ref, routes_ref, own_count):
    return routes_ref[:, pl.ds(pl.multiple_of(tp_ref[0] * own_count, own_count), own_count)]


def dispatch_kernel(
    tp_ref, rows_ref, gain_ref, routes_ref, normed_ref, packed_ref, *, experts, capacity
):
    rows = rows_ref[...].astype(F32)
    inv = lax.rsqrt(jnp.mean(rows * rows, axis=-1, keepdims=True) + norm_eps)
    normed = (rows * inv * gain_ref[...]).astype(BF16)
    normed_ref[...] = normed
    first, second = slot_masks(routes_ref[...], experts, capacity)
    pick = jnp.where(first | second, 1.0, 0.0).astype(BF16)
    packed_ref[...] = jnp.dot(pick, normed, preferred_element_type=F32).astype(BF16)


def dispatch(tp, moe_input, ffn_gain, routes_t, own_count, experts, capacity):
    width = moe_input.shape[1]
    return windowed(
        functools.partial(dispatch_kernel, experts=experts, capacity=capacity),
        (moe_input, ffn_gain.reshape(1, -1), routes_t),
        (
            jax.ShapeDtypeStruct((own_count, width), BF16),
            jax.ShapeDtypeStruct((experts * capacity, width), BF16),
        ),
        (tp,),
        [
            pl.BlockSpec((own_count, width), lambda i, t: (t[0], 0)),
            pl.BlockSpec((1, width), lambda i, t: (0, 0)),
            pl.BlockSpec((2, own_count), lambda i, t: (0, t[0])),
        ],
    )


def combine_kernel(tp_ref, homed_ref, gates_ref, routes_ref, out_ref, *, experts, capacity):
    own_count = out_ref.shape[0]
    first, second = slot_masks(own_routes(tp_ref, routes_ref, own_count), experts, capacity)
    gates = gates_ref[...]
    weights = jnp.where(first, gates[0:1, :], 0.0) + jnp.where(second, gates[1:2, :], 0.0)
    weights = weights.T
    high = weights.astype(BF16)
    low = (weights - high.astype(F32)).astype(BF16)
    homed = homed_ref[...]
    out = jnp.dot(high, homed, preferred_element_type=F32)
    out += jnp.dot(low, homed, preferred_element_type=F32)
    out_ref[...] = out.astype(BF16)


def combine(tp, homed, gates_t, routes_t, own_count, experts, capacity):
    (out,) = call(
        functools.partial(combine_kernel, experts=experts, capacity=capacity),
        (homed, gates_t, routes_t),
        (jax.ShapeDtypeStruct((own_count, homed.shape[1]), BF16),),
        scalars=(tp,),
    )
    return out


def gates_kernel(tp_ref, normed_ref, groups_ref, experts_ref, routes_ref, out_ref):
    normed = normed_ref[...]
    group_logits, expert_logits = (
        lax.dot_general(
            ref[...], normed, (((1,), (1,)), ((), ())), preferred_element_type=F32
        )
        for ref in (groups_ref, experts_ref)
    )
    routes = own_routes(tp_ref, routes_ref, normed.shape[0])
    group_size = expert_logits.shape[0] // group_logits.shape[0]
    groups = lax.broadcasted_iota(jnp.int32, group_logits.shape, 0)
    experts = lax.broadcasted_iota(jnp.int32, expert_logits.shape, 0)
    chosen = routes[0:1, :] // group_size
    own = jnp.sum(jnp.where(groups == chosen, group_logits, 0.0), axis=0, keepdims=True)
    share = 1.0 / jnp.sum(jnp.exp(group_logits - own), axis=0, keepdims=True)
    picked = [
        jnp.sum(jnp.where(experts == routes[k : k + 1, :], expert_logits, 0.0), axis=0, keepdims=True)
        for k in range(2)
    ]
    for k in range(2):
        out_ref[k : k + 1, :] = share / (1.0 + jnp.exp(picked[1 - k] - picked[k]))


def route_gates(tp, normed, group_router, expert_router, routes_t):
    (out,) = call(
        gates_kernel,
        (normed, group_router.T, expert_router.T, routes_t),
        (jax.ShapeDtypeStruct((2, normed.shape[0]), F32),),
        scalars=(tp,),
    )
    return out


def pack_weights_kernel(gate_ref, up_ref, down_ref, top_ref, bottom_ref):
    rows, lanes = gate_ref.shape
    extra = top_ref.shape[0] - rows
    top_ref[:rows, :] = gate_ref[...]
    top_ref[rows:, :] = up_ref[:extra, :]
    bottom_ref[: rows - extra, :] = up_ref[extra:, :]
    at = rows - extra
    for n in range(down_ref.shape[1] // lanes):
        bottom_ref[at : at + lanes, :] = down_ref[:, n * lanes : (n + 1) * lanes]
        at += lanes


def pack_weights(gate, up, down):
    rows, lanes = gate.shape
    shape = jax.ShapeDtypeStruct((3 * rows // 2, lanes), BF16)
    return windowed(pack_weights_kernel, (gate, up, down), (shape, shape), ())


def ffn_kernel(*refs, parts):
    sources, (rows_ref, out_ref, tops, bottoms, acc, sems) = refs[: 2 * parts], refs[2 * parts :]
    model = rows_ref.shape[1]
    lanes = tops.shape[2]
    extra = tops.shape[1] - model
    copies = []
    for n in range(parts):
        for k, (source, held) in enumerate(((sources[n], tops), (sources[parts + n], bottoms))):
            copies.append(pltpu.make_async_copy(source, held.at[n], sems.at[2 * n + k]))
    for copy in copies:
        copy.start()
    rows = rows_ref[...]
    for first in range(0, parts, 2):
        for copy in copies[2 * first : 2 * first + 4]:
            copy.wait()
        pair = (first, first + 1)
        gate = jnp.concatenate([tops[p, :model, :] for p in pair], axis=1)
        up = jnp.concatenate(
            [
                jnp.concatenate([tops[p, model:, :], bottoms[p, : model - extra, :]], axis=0)
                for p in pair
            ],
            axis=1,
        )
        g = jnp.dot(rows, gate, preferred_element_type=F32)
        u = jnp.dot(rows, up, preferred_element_type=F32)
        hidden = (g / (1.0 + jnp.exp(-g)) * u).astype(BF16)
        for n in range(0, model // lanes, 2):
            at = model - extra + n * lanes
            block = jnp.concatenate(
                [
                    jnp.concatenate(
                        [bottoms[p, at : at + lanes, :], bottoms[p, at + lanes : at + 2 * lanes, :]],
                        axis=1,
                    )
                    for p in pair
                ],
                axis=0,
            )
            part = jnp.dot(hidden, block, preferred_element_type=F32)
            to = slice(n * lanes, (n + 2) * lanes)
            if first:
                part += acc[:, to]
            if first + 2 < parts:
                acc[:, to] = part
            else:
                out_ref[:, to] = part.astype(BF16)


def ffn(rows, tops, bottoms):
    parts = len(tops)
    (out,) = call(
        functools.partial(ffn_kernel, parts=parts),
        (rows,),
        (jax.ShapeDtypeStruct(rows.shape, BF16),),
        streamed=(*tops, *bottoms),
        scratch=(
            pltpu.VMEM((parts, *tops[0].shape), BF16),
            pltpu.VMEM((parts, *bottoms[0].shape), BF16),
            pltpu.VMEM(rows.shape, F32),
            pltpu.SemaphoreType.DMA((2 * parts,)),
        ),
        vmem=WIDE,
    )
    return out


def pack_heads_kernel(where_ref, q_ref, k_ref, v_ref, kept_ref, sent_ref, q0_ref, q1_ref):
    _, half, two_depth = kept_ref.shape
    depth = two_depth // 2
    heads = q_ref.shape[1] // depth
    core = where_ref[2]
    for ref, side in ((kept_ref, core), (sent_ref, 1 - core)):
        rows = pl.ds(pl.multiple_of(side * half, half), half)
        for h in range(heads):
            at = slice(h * depth, (h + 1) * depth)
            for copy in range(2):
                ref[2 * h + copy, :, :depth] = k_ref[rows, at]
                ref[2 * h + copy, :, depth:] = v_ref[rows, at]
    late = jnp.where(where_ref[0] >= 4, 1, 0)
    for n, ref in enumerate((q0_ref, q1_ref)):
        h = n + late * (1 - 2 * n)
        ref[...] = q_ref[:, pl.ds(pl.multiple_of(h * depth, depth), depth)]


def query_pairs(n, back=False):
    pairs = []
    for z in range(8):
        for c in range(2):
            j = n if z < 4 else 1 - n
            u = min(z, 7 - z)
            here, there = 2 * z + c, 2 * (2 * (2 * c + j) + u // 2) + u % 2
            pairs.append((there, here) if back else (here, there))
    return pairs


COLUMN_OFFSETS = (0, -1, 1, 2)


def attend_kernel(where_ref, own_ref, other_ref, q0_ref, q1_ref, *refs, columns, scale):
    blocks, (gain_ref, out0_ref, out1_ref, acc, top_ref) = refs[:8], refs[8:]
    z, x, core = where_ref[0], where_ref[1], where_ref[2]
    slices, half, two_depth = blocks[0].shape
    depth = two_depth // 2
    width = depth // 2
    rows = q0_ref.shape[0]
    head = lax.rem(z // 2, 2)
    weight = jnp.where(z // 4 == core, own_ref[head], other_ref[head])
    u = 2 * lax.rem(z, 2) + core

    def folded(a, join):
        return functools.reduce(join, [a[:, n : n + depth] for n in range(0, a.shape[1], depth)])

    def fold(q, number, diagonal):
        block = jnp.concatenate([b[number] for b in blocks], axis=0)
        v = block[:, depth:]
        if diagonal:
            lane = lax.broadcasted_iota(jnp.int32, (rows, half), 1)
            row = lax.broadcasted_iota(jnp.int32, (rows, half), 0) + x * 2 * half
            allowed = []
            for offset in COLUMN_OFFSETS:
                column = lax.rem(x + offset + columns, columns)
                for side in (core, 1 - core):
                    allowed.append(lane + (column * 2 * half + side * half) <= row)
            allowed = jnp.concatenate(allowed, axis=1)
        for m in range(2):
            s = lax.dot_general(
                q[:, m * width : (m + 1) * width],
                block[:, m * width : (m + 1) * width],
                (((1,), (1,)), ((), ())),
                preferred_element_type=F32,
            )
            if diagonal:
                s = jnp.where(allowed, s, masked_score)
            top = jnp.max(folded(s, jnp.maximum), axis=1, keepdims=True)
            if not diagonal:
                old = top_ref[m, :, :1]
                top = jnp.maximum(top, old)
                keep = jnp.exp2((old - top) * scale)
            e = jnp.exp2((s - top) * scale)
            total = folded(e, jnp.add)
            mixed = jnp.dot(e.astype(BF16), v, preferred_element_type=F32)
            if not diagonal:
                mixed = mixed + acc[m, :, :depth] * keep
                total = total + acc[m, :, depth:] * keep
            acc[m, :, :depth] = mixed
            acc[m, :, depth:] = total
            top_ref[m] = jnp.broadcast_to(top, top_ref.shape[1:])

    def one_slice(n, carry):
        q = jnp.where(n == 0, q0_ref[...], q1_ref[...])
        mine = jnp.where(n == head, u, slices - 1 - u)
        fold(q, mine, True)

        def earlier(k, c):
            fold(q, k, False)
            return c

        lax.fori_loop(0, mine, earlier, 0)
        first, second = (
            acc[m, :, :depth] / jnp.sum(acc[m, :, depth:], axis=1, keepdims=True) for m in range(2)
        )
        out = first - weight * second
        out = out * lax.rsqrt(jnp.mean(out * out, axis=1, keepdims=True) + norm_eps)
        out = (out * gain_ref[...]).astype(BF16)
        for chosen, ref in ((0, out0_ref), (1, out1_ref)):

            @pl.when(n == chosen)
            def _(ref=ref):
                ref[...] = out

        return carry

    lax.fori_loop(0, 2, one_slice, 0)


def attend(where, queries, blocks, weights, head_gain, columns, scale):
    rows, depth = queries[0].shape
    out = jax.ShapeDtypeStruct((rows, depth), BF16)
    return call(
        functools.partial(attend_kernel, columns=columns, scale=scale),
        (*queries, *blocks, head_gain.reshape(1, depth)),
        (out, out),
        scalars=(where, *weights),
        scratch=(pltpu.VMEM((2, rows, 2 * depth), F32), pltpu.VMEM((2, rows, depth), F32)),
        vmem=16 * 1024 * 1024,
    )


def local(
    queries,
    keys,
    values,
    lambdas,
    head_gain,
    moe_input,
    ffn_gain,
    group_router,
    expert_router,
    routes,
    w_gate,
    w_up,
    w_down,
):
    z, x, _, core = (lax.axis_index(a) for a in EP_TP)
    tp = lax.axis_index(TP).reshape(1)
    where = jnp.stack([z, x, core])

    top, bottom = pack_weights(w_gate[0], w_up[0], w_down[0])
    top_f = shifted(top, "y", 1)
    bottom_b = shifted(bottom, "y", -1)
    bottom_f = shifted(bottom, "y", 1)
    top_b = shifted(top, "y", -1)
    top_o = shifted(top_f, "y", 1)
    bottom_o = shifted(bottom_b, "y", -1)

    rows = queries.shape[0]
    half = rows // 2
    depth = head_gain.shape[0]
    heads_here = lambdas.shape[0]
    columns = lax.axis_size("x")
    scale = math.log2(math.e) * (depth // 2) ** (-0.5)
    side = jax.ShapeDtypeStruct((2 * heads_here, half, 2 * depth), BF16)
    one_head = jax.ShapeDtypeStruct((rows, depth), BF16)
    kept, sent, q0, q1 = windowed(
        pack_heads_kernel, (queries, keys, values), (side, side, one_head, one_head), (where,)
    )
    got = shifted(sent, "c", 1)
    in_turn = []
    for n, q in enumerate((q0, q1)):
        in_turn.append(lax.ppermute(q, ("z", "c"), query_pairs(n)))
    spread = jnp.where(
        core == 0, jnp.concatenate([kept, got], axis=0), jnp.concatenate([got, kept], axis=0)
    )
    kv = lax.all_to_all(
        spread, "z", split_axis=0, concat_axis=0, tiled=True
    )
    kv_f, kv_b = shifted(kv, "x", 1), shifted(kv, "x", -1)
    kv_o = shifted(kv_f, "x", 1)
    blocks = []
    for block in (kv, kv_f, kv_b, kv_o):
        blocks += [block, shifted(block, "c", 1)]
    weights = (lambdas, shifted(lambdas, "c", 1))

    own_count = routes.shape[0] // lax.axis_size(TP)
    experts = expert_router.shape[1]
    capacity = 2 * own_count // experts
    model_width = moe_input.shape[1]
    routes_t = routes.T
    normed, packed = dispatch(tp, moe_input, ffn_gain, routes_t, own_count, experts, capacity)
    gates_t = route_gates(tp, normed, group_router, expert_router, routes_t)
    arrived = lax.all_to_all(
        packed.reshape(experts, capacity, model_width), EP, split_axis=0, concat_axis=0, tiled=True
    ).reshape(experts * capacity, model_width)
    tops, bottoms = [], []
    for t, b in ((top, bottom), (top_f, bottom_f), (top_b, bottom_b), (top_o, bottom_o)):
        tops += [t, shifted(t, "c", 1)]
        bottoms += [b, shifted(b, "c", 1)]
    results = ffn(arrived, tops, bottoms)
    homed = lax.all_to_all(
        results.reshape(experts, capacity, model_width), EP, split_axis=0, concat_axis=0, tiled=True
    ).reshape(experts * capacity, model_width)

    outgoing = attend(where, in_turn, blocks, weights, head_gain, columns, scale)
    incoming = []
    for n, m in enumerate(outgoing):
        incoming.append(lax.ppermute(m, ("z", "c"), query_pairs(n, back=True)))
    attn_out = jnp.where(
        z < 4, jnp.concatenate(incoming, axis=1), jnp.concatenate(incoming[::-1], axis=1)
    )

    moe_out = combine(tp, homed, gates_t, routes_t, own_count, experts, capacity)
    return (attn_out, moe_out)


def solution(mesh):
    split = Mesh(mesh.devices.reshape(8, 4, 4, 2), EP_TP)
    placed = (
        P(EP, TP),
        P(EP, TP),
        P(EP, TP),
        P(TP),
        P(),
        P(EP, None),
        P(),
        P(),
        P(),
        P(EP, None),
        P(EP, None, TP),
        P(EP, None, TP),
        P(EP, TP, None),
    )

    return jax.shard_map(
        local, mesh=split, in_specs=placed, out_specs=(P(EP, TP), P(EP_TP, None)), check_vma=False
    )
```

```python
import functools
import math

import jax
import jax.numpy as jnp
from jax import lax
from jax.experimental import pallas as pl
from jax.experimental.pallas import tpu as pltpu
from jax.sharding import Mesh
from jax.sharding import PartitionSpec as P


EP = ("z", "x")
EP_TP = ("z", "x", "y", "c")
TP = ("y", "c")

norm_eps = 1e-06
masked_score = -1e30
F32 = jnp.float32
BF16 = jnp.bfloat16
WIDE = 56 * 1024 * 1024


def shifted(array, axis, by):
    n = lax.axis_size(axis)
    return lax.ppermute(array, axis, [(i, (i + by) % n) for i in range(n)])


def windowed(body, args, outs, scalars, specs=None):
    def whole(shape):
        return pl.BlockSpec(shape, lambda *_: (0,) * len(shape))

    return pl.pallas_call(
        body,
        grid_spec=pltpu.PrefetchScalarGridSpec(
            num_scalar_prefetch=len(scalars),
            grid=(1,),
            in_specs=[whole(a.shape) for a in args] if specs is None else specs,
            out_specs=[whole(o.shape) for o in outs],
        ),
        out_shape=list(outs),
        compiler_params=pltpu.CompilerParams(vmem_limit_bytes=WIDE),
    )(*scalars, *args)


def call(body, args, outs, scalars=(), streamed=(), scratch=(), vmem=8 * 1024 * 1024):
    return pl.pallas_call(
        body,
        in_specs=[pl.BlockSpec(memory_space=pltpu.SMEM)] * len(scalars)
        + [pl.BlockSpec(memory_space=pltpu.HBM)] * len(streamed)
        + [pl.BlockSpec(memory_space=pltpu.VMEM)] * len(args),
        out_specs=[pl.BlockSpec(memory_space=pltpu.VMEM)] * len(outs),
        out_shape=list(outs),
        scratch_shapes=list(scratch),
        compiler_params=pltpu.CompilerParams(vmem_limit_bytes=vmem),
    )(*scalars, *streamed, *args)


def slot_masks(routes_t, expert_count, capacity):
    tokens = routes_t.shape[1]
    experts = lax.broadcasted_iota(jnp.int32, (expert_count, tokens), 0)
    named = [routes_t[k : k + 1, :] == experts for k in range(2)]
    both = jnp.where(named[0] | named[1], 1.0, 0.0).astype(BF16)
    earlier = jnp.where(
        lax.broadcasted_iota(jnp.int32, (tokens, tokens), 0)
        < lax.broadcasted_iota(jnp.int32, (tokens, tokens), 1),
        1.0,
        0.0,
    ).astype(BF16)
    rank = jnp.dot(both, earlier, preferred_element_type=F32).astype(jnp.int32)
    place = lax.broadcasted_iota(jnp.int32, (expert_count, capacity, tokens), 1)
    rank = jnp.broadcast_to(rank[:, None, :], place.shape)
    masks = []
    for k in range(2):
        hit = jnp.broadcast_to(jnp.where(named[k], 1, 0)[:, None, :], place.shape)
        masks.append(((hit == 1) & (rank == place)).reshape(expert_count * capacity, tokens))
    return masks


def own_routes(tp_ref, routes_ref, own_count):
    return routes_ref[:, pl.ds(pl.multiple_of(tp_ref[0] * own_count, own_count), own_count)]


def dispatch_kernel(
    tp_ref, rows_ref, gain_ref, routes_ref, normed_ref, packed_ref, *, experts, capacity
):
    rows = rows_ref[...].astype(F32)
    inv = lax.rsqrt(jnp.mean(rows * rows, axis=-1, keepdims=True) + norm_eps)
    normed = (rows * inv * gain_ref[...]).astype(BF16)
    normed_ref[...] = normed
    first, second = slot_masks(routes_ref[...], experts, capacity)
    pick = jnp.where(first | second, 1.0, 0.0).astype(BF16)
    packed_ref[...] = jnp.dot(pick, normed, preferred_element_type=F32).astype(BF16)


def dispatch(tp, moe_input, ffn_gain, routes_t, own_count, experts, capacity):
    width = moe_input.shape[1]
    return windowed(
        functools.partial(dispatch_kernel, experts=experts, capacity=capacity),
        (moe_input, ffn_gain.reshape(1, -1), routes_t),
        (
            jax.ShapeDtypeStruct((own_count, width), BF16),
            jax.ShapeDtypeStruct((experts * capacity, width), BF16),
        ),
        (tp,),
        [
            pl.BlockSpec((own_count, width), lambda i, t: (t[0], 0)),
            pl.BlockSpec((1, width), lambda i, t: (0, 0)),
            pl.BlockSpec((2, own_count), lambda i, t: (0, t[0])),
        ],
    )


def combine_kernel(tp_ref, homed_ref, gates_ref, routes_ref, out_ref, *, experts, capacity):
    own_count = out_ref.shape[0]
    first, second = slot_masks(own_routes(tp_ref, routes_ref, own_count), experts, capacity)
    gates = gates_ref[...]
    weights = jnp.where(first, gates[0:1, :], 0.0) + jnp.where(second, gates[1:2, :], 0.0)
    weights = weights.T
    high = weights.astype(BF16)
    low = (weights - high.astype(F32)).astype(BF16)
    homed = homed_ref[...]
    out = jnp.dot(high, homed, preferred_element_type=F32)
    out += jnp.dot(low, homed, preferred_element_type=F32)
    out_ref[...] = out.astype(BF16)


def combine(tp, homed, gates_t, routes_t, own_count, experts, capacity):
    (out,) = call(
        functools.partial(combine_kernel, experts=experts, capacity=capacity),
        (homed, gates_t, routes_t),
        (jax.ShapeDtypeStruct((own_count, homed.shape[1]), BF16),),
        scalars=(tp,),
    )
    return out


def gates_kernel(tp_ref, normed_ref, groups_ref, experts_ref, routes_ref, out_ref):
    normed = normed_ref[...]
    group_logits, expert_logits = (
        lax.dot_general(
            ref[...], normed, (((1,), (1,)), ((), ())), preferred_element_type=F32
        )
        for ref in (groups_ref, experts_ref)
    )
    routes = own_routes(tp_ref, routes_ref, normed.shape[0])
    group_size = expert_logits.shape[0] // group_logits.shape[0]
    groups = lax.broadcasted_iota(jnp.int32, group_logits.shape, 0)
    experts = lax.broadcasted_iota(jnp.int32, expert_logits.shape, 0)
    chosen = routes[0:1, :] // group_size
    own = jnp.sum(jnp.where(groups == chosen, group_logits, 0.0), axis=0, keepdims=True)
    share = 1.0 / jnp.sum(jnp.exp(group_logits - own), axis=0, keepdims=True)
    picked = [
        jnp.sum(jnp.where(experts == routes[k : k + 1, :], expert_logits, 0.0), axis=0, keepdims=True)
        for k in range(2)
    ]
    for k in range(2):
        out_ref[k : k + 1, :] = share / (1.0 + jnp.exp(picked[1 - k] - picked[k]))


def route_gates(tp, normed, group_router, expert_router, routes_t):
    (out,) = call(
        gates_kernel,
        (normed, group_router.T, expert_router.T, routes_t),
        (jax.ShapeDtypeStruct((2, normed.shape[0]), F32),),
        scalars=(tp,),
    )
    return out


def pack_weights_kernel(gate_ref, up_ref, down_ref, top_ref, bottom_ref):
    rows, lanes = gate_ref.shape
    extra = top_ref.shape[0] - rows
    top_ref[:rows, :] = gate_ref[...]
    top_ref[rows:, :] = up_ref[:extra, :]
    bottom_ref[: rows - extra, :] = up_ref[extra:, :]
    at = rows - extra
    for n in range(down_ref.shape[1] // lanes):
        bottom_ref[at : at + lanes, :] = down_ref[:, n * lanes : (n + 1) * lanes]
        at += lanes


def pack_weights(gate, up, down):
    rows, lanes = gate.shape
    shape = jax.ShapeDtypeStruct((3 * rows // 2, lanes), BF16)
    return windowed(pack_weights_kernel, (gate, up, down), (shape, shape), ())


def ffn_kernel(rows_in, *refs, parts):
    sources, (out_ref, rows_ref, tops, bottoms, acc, sems) = refs[: 2 * parts], refs[2 * parts :]
    model = rows_ref.shape[1]
    lanes = tops.shape[2]
    extra = tops.shape[1] - model
    copies = []
    for n in range(parts):
        for k, (source, held) in enumerate(((sources[n], tops), (sources[parts + n], bottoms))):
            copies.append(pltpu.make_async_copy(source, held.at[n], sems.at[2 * n + k]))
    rows_copy = pltpu.make_async_copy(rows_in, rows_ref, sems.at[2 * parts])
    rows_copy.start()
    for copy in copies[:8]:
        copy.start()
    rows_copy.wait()
    rows = rows_ref[...]
    for first in range(0, parts, 2):
        for copy in copies[2 * first : 2 * first + 4]:
            copy.wait()
        for copy in copies[2 * first + 8 : 2 * first + 12]:
            copy.start()
        pair = (first, first + 1)
        gate = jnp.concatenate([tops[p, :model, :] for p in pair], axis=1)
        up = jnp.concatenate(
            [
                jnp.concatenate([tops[p, model:, :], bottoms[p, : model - extra, :]], axis=0)
                for p in pair
            ],
            axis=1,
        )
        g = jnp.dot(rows, gate, preferred_element_type=F32)
        u = jnp.dot(rows, up, preferred_element_type=F32)
        hidden = (g / (1.0 + jnp.exp(-g)) * u).astype(BF16)
        for n in range(0, model // lanes, 2):
            at = model - extra + n * lanes
            block = jnp.concatenate(
                [
                    jnp.concatenate(
                        [bottoms[p, at : at + lanes, :], bottoms[p, at + lanes : at + 2 * lanes, :]],
                        axis=1,
                    )
                    for p in pair
                ],
                axis=0,
            )
            part = jnp.dot(hidden, block, preferred_element_type=F32)
            to = slice(n * lanes, (n + 2) * lanes)
            if first:
                part += acc[:, to]
            if first + 2 < parts:
                acc[:, to] = part
            else:
                out_ref[:, to] = part.astype(BF16)


def ffn(rows, tops, bottoms):
    parts = len(tops)
    (out,) = call(
        functools.partial(ffn_kernel, parts=parts),
        (),
        (jax.ShapeDtypeStruct(rows.shape, BF16),),
        streamed=(rows, *tops, *bottoms),
        scratch=(
            pltpu.VMEM(rows.shape, BF16),
            pltpu.VMEM((parts, *tops[0].shape), BF16),
            pltpu.VMEM((parts, *bottoms[0].shape), BF16),
            pltpu.VMEM(rows.shape, F32),
            pltpu.SemaphoreType.DMA((2 * parts + 1,)),
        ),
        vmem=56 * 1024 * 1024,
    )
    return out


def pack_heads_kernel(q_ref, k_ref, v_ref, kept_ref, sent_ref, q0_ref, q1_ref):
    _, half, two_depth = kept_ref.shape
    depth = two_depth // 2
    heads = q_ref.shape[1] // depth
    core = lax.axis_index("c")
    for ref, side in ((kept_ref, core), (sent_ref, 1 - core)):
        rows = pl.ds(pl.multiple_of(side * half, half), half)
        for h in range(heads):
            at = slice(h * depth, (h + 1) * depth)
            for copy in range(2):
                ref[2 * h + copy, :, :depth] = k_ref[rows, at]
                ref[2 * h + copy, :, depth:] = v_ref[rows, at]
    late = jnp.where(lax.axis_index("z") >= 4, 1, 0)
    for n, ref in enumerate((q0_ref, q1_ref)):
        h = n + late * (1 - 2 * n)
        ref[...] = q_ref[:, pl.ds(pl.multiple_of(h * depth, depth), depth)]


def query_pairs(n, back=False):
    pairs = []
    for z in range(8):
        for c in range(2):
            j = n if z < 4 else 1 - n
            u = min(z, 7 - z)
            here, there = 2 * z + c, 2 * (2 * (2 * c + j) + u // 2) + u % 2
            pairs.append((there, here) if back else (here, there))
    return pairs


COLUMN_OFFSETS = (0, -1, 1, 2)


def attend_kernel(own_ref, other_ref, q0_ref, q1_ref, *refs, columns, scale):
    blocks, (gain_ref, out0_ref, out1_ref, acc, top_ref) = refs[:8], refs[8:]
    z, x, core = (lax.axis_index(a) for a in ("z", "x", "c"))
    slices, half, two_depth = blocks[0].shape
    depth = two_depth // 2
    width = depth // 2
    rows = q0_ref.shape[0]
    head = lax.rem(z // 2, 2)
    weight = jnp.where(z // 4 == core, own_ref[head], other_ref[head])
    u = 2 * lax.rem(z, 2) + core

    def folded(a, join):
        return functools.reduce(join, [a[:, n : n + depth] for n in range(0, a.shape[1], depth)])

    def fold(q, number, diagonal):
        block = jnp.concatenate([b[number] for b in blocks], axis=0)
        v = block[:, depth:]
        if diagonal:
            lane = lax.broadcasted_iota(jnp.int32, (rows, half), 1)
            row = lax.broadcasted_iota(jnp.int32, (rows, half), 0) + x * 2 * half
            allowed = []
            for offset in COLUMN_OFFSETS:
                column = lax.rem(x + offset + columns, columns)
                for side in (core, 1 - core):
                    allowed.append(lane + (column * 2 * half + side * half) <= row)
            allowed = jnp.concatenate(allowed, axis=1)
        for m in range(2):
            s = lax.dot_general(
                q[:, m * width : (m + 1) * width],
                block[:, m * width : (m + 1) * width],
                (((1,), (1,)), ((), ())),
                preferred_element_type=F32,
            )
            if diagonal:
                s = jnp.where(allowed, s, masked_score)
            top = jnp.max(folded(s, jnp.maximum), axis=1, keepdims=True)
            if not diagonal:
                old = top_ref[m, :, :1]
                top = jnp.maximum(top, old)
                keep = jnp.exp2((old - top) * scale)
            e = jnp.exp2((s - top) * scale)
            total = folded(e, jnp.add)
            mixed = jnp.dot(e.astype(BF16), v, preferred_element_type=F32)
            if not diagonal:
                mixed = mixed + acc[m, :, :depth] * keep
                total = total + acc[m, :, depth:] * keep
            acc[m, :, :depth] = mixed
            acc[m, :, depth:] = total
            top_ref[m] = jnp.broadcast_to(top, top_ref.shape[1:])

    def one_slice(n, carry):
        q = jnp.where(n == 0, q0_ref[...], q1_ref[...])
        mine = jnp.where(n == head, u, slices - 1 - u)
        fold(q, mine, True)

        def earlier(k, c):
            fold(q, k, False)
            return c

        lax.fori_loop(0, mine, earlier, 0)
        first, second = (
            acc[m, :, :depth] / jnp.sum(acc[m, :, depth:], axis=1, keepdims=True) for m in range(2)
        )
        out = first - weight * second
        out = out * lax.rsqrt(jnp.mean(out * out, axis=1, keepdims=True) + norm_eps)
        out = (out * gain_ref[...]).astype(BF16)
        for chosen, ref in ((0, out0_ref), (1, out1_ref)):

            @pl.when(n == chosen)
            def _(ref=ref):
                ref[...] = out

        return carry

    lax.fori_loop(0, 2, one_slice, 0)


def attend(queries, blocks, weights, head_gain, columns, scale):
    rows, depth = queries[0].shape
    out = jax.ShapeDtypeStruct((rows, depth), BF16)
    return call(
        functools.partial(attend_kernel, columns=columns, scale=scale),
        (*queries, *blocks, head_gain.reshape(1, depth)),
        (out, out),
        scalars=weights,
        scratch=(pltpu.VMEM((2, rows, 2 * depth), F32), pltpu.VMEM((2, rows, depth), F32)),
        vmem=16 * 1024 * 1024,
    )


def local(
    queries,
    keys,
    values,
    lambdas,
    head_gain,
    moe_input,
    ffn_gain,
    group_router,
    expert_router,
    routes,
    w_gate,
    w_up,
    w_down,
):
    z, _, _, core = (lax.axis_index(a) for a in EP_TP)
    tp = lax.axis_index(TP).reshape(1)

    top, bottom = pack_weights(w_gate[0], w_up[0], w_down[0])
    top_f = shifted(top, "y", 1)
    bottom_b = shifted(bottom, "y", -1)
    bottom_f = shifted(bottom, "y", 1)
    top_b = shifted(top, "y", -1)
    top_o = shifted(top_f, "y", 1)
    bottom_o = shifted(bottom_b, "y", -1)

    rows = queries.shape[0]
    half = rows // 2
    depth = head_gain.shape[0]
    heads_here = lambdas.shape[0]
    columns = lax.axis_size("x")
    scale = math.log2(math.e) * (depth // 2) ** (-0.5)
    side = jax.ShapeDtypeStruct((2 * heads_here, half, 2 * depth), BF16)
    one_head = jax.ShapeDtypeStruct((rows, depth), BF16)
    kept, sent, q0, q1 = windowed(
        pack_heads_kernel, (queries, keys, values), (side, side, one_head, one_head), ()
    )
    got = shifted(sent, "c", 1)
    in_turn = []
    for n, q in enumerate((q0, q1)):
        in_turn.append(lax.ppermute(q, ("z", "c"), query_pairs(n)))
    spread = jnp.where(
        core == 0, jnp.concatenate([kept, got], axis=0), jnp.concatenate([got, kept], axis=0)
    )
    kv = lax.all_to_all(
        spread, "z", split_axis=0, concat_axis=0, tiled=True
    )
    kv_f, kv_b = shifted(kv, "x", 1), shifted(kv, "x", -1)
    kv_o = shifted(kv_f, "x", 1)
    blocks = []
    for block in (kv, kv_f, kv_b, kv_o):
        blocks += [block, shifted(block, "c", 1)]
    weights = (lambdas, shifted(lambdas, "c", 1))

    own_count = routes.shape[0] // lax.axis_size(TP)
    experts = expert_router.shape[1]
    capacity = 2 * own_count // experts
    model_width = moe_input.shape[1]
    routes_t = routes.T
    normed, packed = dispatch(tp, moe_input, ffn_gain, routes_t, own_count, experts, capacity)
    gates_t = route_gates(tp, normed, group_router, expert_router, routes_t)
    arrived = lax.all_to_all(
        packed.reshape(experts, capacity, model_width), EP, split_axis=0, concat_axis=0, tiled=True
    ).reshape(experts * capacity, model_width)
    tops, bottoms = [], []
    for t, b in ((top, bottom), (top_f, bottom_f), (top_b, bottom_b), (top_o, bottom_o)):
        tops += [t, shifted(t, "c", 1)]
        bottoms += [b, shifted(b, "c", 1)]
    results = ffn(arrived, tops, bottoms)
    homed = lax.all_to_all(
        results.reshape(experts, capacity, model_width), EP, split_axis=0, concat_axis=0, tiled=True
    ).reshape(experts * capacity, model_width)

    outgoing = attend(in_turn, blocks, weights, head_gain, columns, scale)
    incoming = []
    for n, m in enumerate(outgoing):
        incoming.append(lax.ppermute(m, ("z", "c"), query_pairs(n, back=True)))
    attn_out = jnp.where(
        z < 4, jnp.concatenate(incoming, axis=1), jnp.concatenate(incoming[::-1], axis=1)
    )

    moe_out = combine(tp, homed, gates_t, routes_t, own_count, experts, capacity)
    return (attn_out, moe_out)


def solution(mesh):
    split = Mesh(mesh.devices.reshape(8, 4, 4, 2), EP_TP)
    placed = (
        P(EP, TP),
        P(EP, TP),
        P(EP, TP),
        P(TP),
        P(),
        P(EP, None),
        P(),
        P(),
        P(),
        P(EP, None),
        P(EP, None, TP),
        P(EP, None, TP),
        P(EP, TP, None),
    )

    return jax.shard_map(
        local, mesh=split, in_specs=placed, out_specs=(P(EP, TP), P(EP_TP, None)), check_vma=False
    )
```
